32 devices in a mesh: sp: 8 (over z, x), tp: 4 (over y, core).
Axes of the slice: x: 2, y: 2, z: 4, core: 2. Of those that a mesh axis runs over, the one named last changes fastest.
Arguments:
- residual: bfloat16 [6144, 2048], P('sp'), may hold values from -6 to 6
- query_matrix: bfloat16 [6144, 1024], P('sp', 'tp'), may hold values from -6 to 6
- key_matrix: bfloat16 [6144, 1024], P('sp', 'tp'), may hold values from -6 to 6
- value_matrix: bfloat16 [6144, 2048], P('sp', 'tp'), may hold values from -6 to 6
- output_gate_logit: bfloat16 [6144, 2048], P('sp', 'tp'), may hold values from -6 to 6
- input_gate_log: float32 [6144, 8], P('sp', 'tp'), may hold values from -4 to 125
- forget_gate_logit: float32 [6144, 8], P('sp', 'tp')
- extra_head_decay: float32 [6144, 8], P('sp', 'tp'), may hold values from -1 to 0
- head_norm_gain: float32 [2048], P('tp'), may hold values from 0.1 to 1.9
- projection: bfloat16 [2048, 2048], P('tp'), may hold values from -5.303301 to 5.303301
- cell_output_gain: float32 [2048], replicated, may hold values from 0.1 to 1.9
- mixer_input_gain: float32 [2048], replicated, may hold values from 0.1 to 1.9
- mixer_gate_weight: bfloat16 [2048, 5120], P('sp', 'tp'), may hold values from -0.125 to 0.125
- mixer_up_weight: bfloat16 [2048, 5120], P('sp', 'tp'), may hold values from -0.125 to 0.125
- mixer_down_weight: bfloat16 [5120, 2048], P('tp', 'sp'), may hold values from -0.078125 to 0.078125
Outputs:
- updated: bfloat16 [6144, 2048], P('sp', 'tp')
The draws below stay inside these ranges and needn't reach their ends.
All inputs are finite; a program needn't handle non-finite values.
Results may differ from the reference program's by a relative error of at most 0.014.
Values may be sent and summed in bfloat16 or wider, within the bound.
A program may use at most 128 MiB of HBM per device.

```python
import math
import jax
import jax.numpy as jnp
from jax import lax

D = 2048
HEADS = 8
DQK = 128
DV = 256
FF = 5120
TOK_DEV = 768
TOKENS = 6144
M_V = 2048
N_TP = 4


def draw_input_gate_log(key, part):
    values = jnp.clip(jax.random.normal(key, (TOKENS, HEADS), jnp.float32), -4.0, 4.0)
    return values


def draw_forget_gate_logit(key, part):
    slow_limit = 5
    slow = jax.random.randint(jax.random.fold_in(key, 1), (HEADS,), 0, 10) < slow_limit
    quick = jnp.log(jax.random.uniform(jax.random.fold_in(key, 2), (HEADS,), jnp.float32, 30.0, 60.0))
    level = jnp.where(slow, jnp.log(4.0 * TOKENS), quick)
    shifts = jax.random.uniform(jax.random.fold_in(key, 3), (TOKENS // TOK_DEV, HEADS), jnp.float32, -0.7, 0.7)
    shifts = jnp.repeat(shifts, TOK_DEV, axis=0)
    noise = jnp.clip(jax.random.normal(jax.random.fold_in(key, 4), (TOKENS, HEADS), jnp.float32), -4.0, 4.0)
    return level[None, :] + shifts + noise


def draw_extra_head_decay(key, part):
    spots = jax.random.randint(jax.random.fold_in(key, 1), (3, HEADS), 0, TOKENS)
    depth = jnp.log(jax.random.uniform(jax.random.fold_in(key, 2), (3, HEADS), jnp.float32, 0.5, 0.8))
    columns = lax.broadcasted_iota(jnp.int32, (3, HEADS), 1)
    return jnp.zeros((TOKENS, HEADS), jnp.float32).at[spots, columns].set(depth)


def draw_projection(key, part):
    base = jnp.clip(jax.random.normal(key, (M_V, D), jnp.float32), -6.0, 6.0) * M_V ** (-0.5)
    position = lax.broadcasted_iota(jnp.float32, (1, D), 1) / D
    jitter = jnp.exp(jax.random.uniform(jax.random.fold_in(key, 3), (1, D), jnp.float32, -0.35, 0.35))
    return (base * jnp.exp(1.0986 * position) * jitter).astype(jnp.bfloat16)


def level_of(rng, extent, shards, smallest, top_value):
    loudness = 1.0
    for axis_at, blocks in shards:
        steps = jax.random.uniform(jax.random.fold_in(jax.random.fold_in(rng, 6), axis_at), (blocks,), jnp.float32, smallest / len(shards), top_value / len(shards))
        loudness = loudness * jnp.repeat(jnp.exp(steps), extent[axis_at] // blocks).reshape((-1,) + (1,) * (len(extent) - 1 - axis_at))
    return loudness


def centred(stream_key, dims, scale, reach, cuts=(), kind=jnp.bfloat16):
    values = jax.random.normal(stream_key, dims, jnp.float32) * scale
    if len(cuts) > 0:
        values = level_of(stream_key, dims, cuts, -0.22, 0.18) * values
    return jnp.clip(values, min=-reach, max=reach).astype(kind)


def setup_inputs(seed: int = 0) -> dict:
    arg_keys = jax.random.split(jax.random.key(seed), 16)
    return {
        "residual": centred(arg_keys[0], (TOKENS, D), 1.0, 6.0, ((0, 8),)),
        "query_matrix": centred(arg_keys[1], (TOKENS, HEADS * DQK), 1.0, 6.0, ((0, 8), (1, 4))),
        "key_matrix": centred(arg_keys[2], (TOKENS, HEADS * DQK), 1.0, 6.0, ((0, 8), (1, 4))),
        "value_matrix": centred(arg_keys[3], (TOKENS, M_V), 1.0, 6.0, ((0, 8), (1, 4))),
        "output_gate_logit": centred(arg_keys[4], (TOKENS, M_V), 1.0, 6.0, ((0, 8), (1, 4))),
        "input_gate_log": draw_input_gate_log(jax.random.fold_in(arg_keys[15], 71), 0),
        "forget_gate_logit": draw_forget_gate_logit(jax.random.fold_in(arg_keys[15], 71), 0),
        "extra_head_decay": draw_extra_head_decay(jax.random.fold_in(arg_keys[15], 71), 0),
        "head_norm_gain": jnp.clip(1.0 + 0.18 * jax.random.normal(arg_keys[8], (M_V,), jnp.float32), 0.1, 1.9),
        "projection": draw_projection(jax.random.fold_in(arg_keys[15], 71), 0),
        "cell_output_gain": jnp.clip(1.0 + 0.18 * jax.random.normal(arg_keys[10], (D,), jnp.float32), 0.1, 1.9),
        "mixer_input_gain": jnp.clip(1.0 + 0.18 * jax.random.normal(arg_keys[11], (D,), jnp.float32), 0.1, 1.9),
        "mixer_gate_weight": centred(arg_keys[12], (D, FF), D ** -0.5, 0.125, ((0, 8), (1, 4))),
        "mixer_up_weight": centred(arg_keys[13], (D, FF), D ** -0.5, 0.125, ((0, 8), (1, 4))),
        "mixer_down_weight": centred(arg_keys[14], (FF, D), FF ** -0.5, 0.078125, ((0, 4), (1, 8))),
    }


HIGHEST = lax.Precision.HIGHEST
EPSILON = 1e-06

def read_out(query, keyed, valued, in_logs, running_log_total, memory, normalizer, stabilizer):
    length = query.shape[1]
    causal = lax.broadcasted_iota(jnp.int32, (length, length), 0) >= lax.broadcasted_iota(jnp.int32, (length, length), 1)
    spread = running_log_total[:, :, None] - running_log_total[:, None, :] + in_logs[:, None, :]
    spread = jnp.where(causal[None], spread, -jnp.inf)
    carried = running_log_total + stabilizer[:, None]
    running = jnp.maximum(carried, lax.optimization_barrier(jnp.max(spread, axis=-1)))
    scores = jnp.einsum('htd,hsd->hts', query, keyed, precision=HIGHEST) * DQK ** (-0.5)
    weights = jnp.exp(spread - running[:, :, None]) * scores
    weight_low = lax.optimization_barrier(weights.astype(jnp.bfloat16)).astype(jnp.float32)
    scaled = jnp.exp(carried - running)
    scaled_query = query * DQK ** (-0.5)
    numerator = jnp.einsum('hts,hsv->htv', weight_low, valued, precision=HIGHEST)
    numerator = numerator + scaled[:, :, None] * jnp.einsum('hvd,htd->htv', memory, scaled_query, precision=HIGHEST)
    denominator = lax.optimization_barrier(jnp.sum(weights, axis=-1)) + scaled * jnp.einsum('hd,htd->ht', normalizer, scaled_query, precision=HIGHEST)
    return numerator / jnp.maximum(jnp.abs(denominator), jnp.exp(-running))[:, :, None]

def fold_state(keyed, valued, in_logs, running_log_total, memory, normalizer, stabilizer):
    last = running_log_total[:, -1]
    lifted = last[:, None] - running_log_total + in_logs
    new_max = jnp.maximum(last + stabilizer, lax.optimization_barrier(jnp.max(lifted, axis=-1)))
    weights = jnp.exp(lifted - new_max[:, None])
    retained = jnp.exp(last + stabilizer - new_max)
    memory = retained[:, None, None] * memory + jnp.einsum('hsv,hsd->hvd', weights[:, :, None] * valued, keyed, precision=HIGHEST)
    normalizer = retained[:, None] * normalizer + jnp.einsum('hs,hsd->hd', weights, keyed, precision=HIGHEST)
    return (memory, normalizer, new_max)

def block_sum(left, right, parts):
    rows = left.shape[0]
    inner = left.shape[1] // parts
    left_blocks = left.reshape(rows, parts, inner).transpose(1, 0, 2)
    right_blocks = right.reshape(parts, inner, right.shape[1])

    def accumulate(total, pair):
        product = jnp.dot(pair[0], pair[1], preferred_element_type=jnp.float32).astype(jnp.bfloat16)
        return (total + lax.optimization_barrier(product).astype(jnp.float32), None)
    total, unused = lax.scan(accumulate, jnp.zeros((rows, right.shape[1]), jnp.float32), (left_blocks, right_blocks))
    return total

def reference(residual, query_matrix, key_matrix, value_matrix, output_gate_logit, input_gate_log, forget_gate_logit, extra_head_decay, head_norm_gain, projection, cell_output_gain, mixer_input_gain, mixer_gate_weight, mixer_up_weight, mixer_down_weight):
    span = math.gcd(TOKENS, 512)
    count = TOKENS // span

    def arrange(array, width):
        return array.astype(jnp.float32).reshape(count, span, HEADS, width).transpose(0, 2, 1, 3)
    query = arrange(query_matrix, DQK)
    keyed = arrange(key_matrix, DQK)
    valued = arrange(value_matrix, DV)
    in_logs = input_gate_log.reshape(count, span, HEADS).transpose(0, 2, 1)
    forget_log_value = jax.nn.log_sigmoid(forget_gate_logit) + extra_head_decay
    running_log_total = jnp.cumsum(forget_log_value.reshape(count, span, HEADS), axis=1).transpose(0, 2, 1)

    def advance(state, blocks):
        memory, normalizer, stabilizer = state
        query_block, key_block, value_block, gate_block, decay_block = blocks
        cells = read_out(query_block, key_block, value_block, gate_block, decay_block, memory, normalizer, stabilizer)
        return (fold_state(key_block, value_block, gate_block, decay_block, memory, normalizer, stabilizer), cells)
    start = (jnp.zeros((HEADS, DV, DQK), jnp.float32), jnp.zeros((HEADS, DQK), jnp.float32), jnp.zeros((HEADS,), jnp.float32))
    unused, cells = lax.scan(advance, start, (query, keyed, valued, in_logs, running_log_total))
    centered = cells - lax.optimization_barrier(jnp.mean(cells, axis=-1, keepdims=True))
    normed = centered * lax.rsqrt(lax.optimization_barrier(jnp.mean(centered * centered, axis=-1, keepdims=True)) + EPSILON)
    normed = normed * head_norm_gain.reshape(HEADS, DV)[None, :, None, :]
    normed = normed.transpose(0, 2, 1, 3).reshape(TOKENS, HEADS * DV)
    gated = (normed * jax.nn.sigmoid(output_gate_logit.astype(jnp.float32))).astype(jnp.bfloat16)
    mixed = block_sum(gated, projection, N_TP)
    mixed = mixed * lax.rsqrt(lax.optimization_barrier(jnp.mean(mixed * mixed, axis=-1, keepdims=True)) + EPSILON) * cell_output_gain
    first_sum = (residual.astype(jnp.float32) + mixed).astype(jnp.bfloat16)
    first_wide = lax.optimization_barrier(first_sum).astype(jnp.float32)
    normed_rows = (first_wide * lax.rsqrt(lax.optimization_barrier(jnp.mean(first_wide * first_wide, axis=-1, keepdims=True)) + EPSILON) * mixer_input_gain).astype(jnp.bfloat16)
    gate_value = jnp.dot(normed_rows, mixer_gate_weight, preferred_element_type=jnp.float32)
    up_value = jnp.dot(normed_rows, mixer_up_weight, preferred_element_type=jnp.float32)
    activated = (jax.nn.silu(gate_value) * up_value).astype(jnp.bfloat16)
    channel_out = block_sum(activated, mixer_down_weight, N_TP)
    return (first_wide + 0.5 * channel_out).astype(jnp.bfloat16)
```

```python
import functools

import jax
import jax.numpy as jnp
from jax import lax
from jax.experimental import pallas as pl
from jax.experimental.pallas import tpu as pltpu
from jax.sharding import PartitionSpec as P

DQK = 128
DV = 256
MESH = pl.DeviceIdType.MESH
VMEM = pl.BlockSpec(memory_space=pltpu.VMEM)
ANY = pl.BlockSpec(memory_space=pl.ANY)
VMEM_BYTES = 60 * 1024 * 1024


HIGHEST = lax.Precision.HIGHEST
EPSILON = 1e-06
LOWEST_LOG = -1e30


def heads_first(array, heads, width):
    return array.reshape(array.shape[0], heads, width).transpose(1, 0, 2)


def read_out(
    query_low, key_low, value_low, in_logs, running_log_total, memory, normalizer, stabilizer
):
    length = query_low.shape[1]
    causal = lax.broadcasted_iota(jnp.int32, (length, length), 0) >= lax.broadcasted_iota(
        jnp.int32, (length, length), 1
    )
    spread = running_log_total[:, :, None] - running_log_total[:, None, :] + in_logs[:, None, :]
    spread = jnp.where(causal[None], spread, -jnp.inf)
    carried = running_log_total + stabilizer[:, None]
    running = jnp.maximum(carried, jnp.max(spread, axis=-1))
    scores = jnp.einsum(
        "htd,hsd->hts", query_low, key_low, preferred_element_type=jnp.float32
    ) * DQK ** (-0.5)
    weights = jnp.exp(spread - running[:, :, None]) * scores
    scaled = jnp.exp(carried - running)
    scaled_query = query_low.astype(jnp.float32) * DQK ** (-0.5)
    numerator = jnp.einsum(
        "hts,hsv->htv", weights.astype(jnp.bfloat16), value_low, preferred_element_type=jnp.float32
    )
    numerator = numerator + scaled[:, :, None] * jnp.einsum(
        "hvd,htd->htv", memory, scaled_query, precision=HIGHEST
    )
    denominator = jnp.sum(weights, axis=-1) + scaled * jnp.einsum(
        "hd,htd->ht", normalizer, scaled_query, precision=HIGHEST
    )
    return numerator / jnp.maximum(jnp.abs(denominator), jnp.exp(-running))[:, :, None]


def fold_state(keyed, valued, in_logs, running_log_total, memory, normalizer, stabilizer):
    last = running_log_total[:, -1]
    lifted = last[:, None] - running_log_total + in_logs
    new_max = jnp.maximum(last + stabilizer, jnp.max(lifted, axis=-1))
    weights = jnp.exp(lifted - new_max[:, None])
    retained = jnp.exp(last + stabilizer - new_max)
    memory = retained[:, None, None] * memory + jnp.einsum(
        "hsv,hsd->hvd", weights[:, :, None] * valued, keyed, precision=HIGHEST
    )
    normalizer = retained[:, None] * normalizer + jnp.einsum(
        "hs,hsd->hd", weights, keyed, precision=HIGHEST
    )
    return (memory, normalizer, new_max)


def greet(axis, count):
    me = lax.axis_index(axis)
    barrier = pltpu.get_barrier_semaphore()
    for step in range(1, count):
        pl.semaphore_signal(
            barrier, inc=1, device_id={axis: lax.rem(me + step, count)}, device_id_type=MESH
        )
    pl.semaphore_wait(barrier, count - 1)


def prior_kernel(count, heads, memory_ref, aux_ref, out_ref, out_aux, slots, aux_slots, sems):
    me = lax.axis_index("sp")
    greet("sp", count)

    def copies(step):
        peer = {"sp": lax.rem(me + step, count)}
        return (
            pltpu.make_async_remote_copy(
                memory_ref, slots.at[step - 1], sems.at[0, step - 1], sems.at[1, step - 1],
                device_id=peer, device_id_type=MESH,
            ),
            pltpu.make_async_remote_copy(
                aux_ref, aux_slots.at[step - 1], sems.at[2, step - 1], sems.at[3, step - 1],
                device_id=peer, device_id_type=MESH,
            ),
        )

    for step in range(1, count):

        @pl.when(me + step < count)
        def _():
            for copy in copies(step):
                copy.start()

    out_ref[...] = jnp.zeros_like(out_ref)
    out_aux[...] = jnp.zeros_like(out_aux)
    out_aux[heads : 2 * heads, :] = jnp.full((heads, DQK), LOWEST_LOG, jnp.float32)
    for step in range(count - 1, 0, -1):

        @pl.when(me >= step)
        def _():
            for copy in copies(step):
                copy.wait_recv()
            late = aux_slots[step - 1]
            for head in range(heads):
                rows = pl.ds(head * DV, DV)
                early_max = out_aux[heads + head : heads + head + 1, :]
                late_max = late[heads + head : heads + head + 1, :]
                late_decay = late[2 * heads + head : 2 * heads + head + 1, :]
                joined = jnp.maximum(late_decay + early_max, late_max)
                first = jnp.exp(late_decay + early_max - joined)
                second = jnp.exp(late_max - joined)
                out_ref[rows, :] = first * out_ref[rows, :] + second * slots[
                    step - 1, rows, :
                ].astype(jnp.float32)
                out_aux[head : head + 1, :] = (
                    first * out_aux[head : head + 1, :] + second * late[head : head + 1, :]
                )
                out_aux[heads + head : heads + head + 1, :] = joined
                out_aux[2 * heads + head : 2 * heads + head + 1, :] = (
                    out_aux[2 * heads + head : 2 * heads + head + 1, :] + late_decay
                )

    for step in range(1, count):

        @pl.when(me + step < count)
        def _():
            for copy in copies(step):
                copy.wait_send()


def prior_states(decay, memory, normalizer, maximum):
    count = lax.axis_size("sp")
    heads = decay.shape[0]
    spread = lambda row: jnp.broadcast_to(row[:, None], (heads, DQK))
    aux = jnp.concatenate([normalizer, spread(maximum), spread(decay)])
    height = -(-3 * heads // 8) * 8
    aux = jnp.pad(aux, ((0, height - 3 * heads), (0, 0)))
    low = memory.reshape(heads * DV, DQK).astype(jnp.bfloat16)
    prior, aux = pl.pallas_call(
        functools.partial(prior_kernel, count, heads),
        out_shape=(
            jax.ShapeDtypeStruct((heads * DV, DQK), jnp.float32),
            jax.ShapeDtypeStruct((height, DQK), jnp.float32),
        ),
        in_specs=[VMEM] * 2,
        out_specs=(VMEM, VMEM),
        scratch_shapes=[
            pltpu.VMEM((count - 1, heads * DV, DQK), jnp.bfloat16),
            pltpu.VMEM((count - 1, height, DQK), jnp.float32),
            pltpu.SemaphoreType.DMA((4, count - 1)),
        ],
        compiler_params=pltpu.CompilerParams(collective_id=0, has_side_effects=True),
        cost_estimate=pl.CostEstimate(flops=10**9, bytes_accessed=40 * 10**6, transcendentals=0),
        name="prior",
    )(low, aux)
    return (
        aux[2 * heads : 3 * heads, 0],
        prior.reshape(heads, DV, DQK),
        aux[:heads],
        aux[heads : 2 * heads, 0],
    )


def project_kernel(
    count, pieces, tile, gated_ref, residual_ref, out_gain, in_gain, *refs
):
    weight_refs = refs[:pieces]
    normed_ref, own_ref, blocks, weight, first, sems, weight_sem = refs[pieces:]
    me = lax.axis_index("tp")
    depth = gated_ref.shape[1]
    rows_all, width = residual_ref.shape
    for ref, index in zip(weight_refs, tp_order(count, pieces)):
        start = pl.multiple_of(index * depth, depth)
        pltpu.make_async_copy(
            ref, weight.at[pl.ds(start, ref.shape[0]), :], weight_sem
        ).start()
    greet("tp", count)
    copies = []
    for step in range(count - 1, 0, -1):
        copies.append(
            pltpu.make_async_remote_copy(
                gated_ref, blocks.at[me], sems.at[0, step - 1], sems.at[1, step - 1],
                device_id={"tp": lax.rem(me + step, count)}, device_id_type=MESH,
            )
        )
        copies[-1].start()
    blocks[me] = gated_ref[...]
    pltpu.make_async_copy(weight, weight, weight_sem).wait()
    for copy in copies:
        copy.wait_recv()

    def turn(at, unused):
        rows = pl.ds(pl.multiple_of(at * tile, tile), tile)
        mixed = jnp.zeros((tile, width), jnp.float32)
        for block in range(count):
            mixed = mixed + jnp.dot(
                blocks[block, rows, :],
                weight[block * depth : (block + 1) * depth, :],
                preferred_element_type=jnp.float32,
            )
        scale = lax.rsqrt(jnp.mean(mixed * mixed, axis=-1, keepdims=True) + EPSILON)
        total = residual_ref[rows, :].astype(jnp.float32) + mixed * scale * out_gain[...]
        total = total.astype(jnp.bfloat16)
        first[rows, :] = total
        wide = total.astype(jnp.float32)
        scale = lax.rsqrt(jnp.mean(wide * wide, axis=-1, keepdims=True) + EPSILON)
        normed_ref[rows, :] = (wide * scale * in_gain[...]).astype(jnp.bfloat16)
        return unused

    lax.fori_loop(0, rows_all // tile, turn, 0)
    cols = width // count
    own_ref[...] = first[:, pl.ds(pl.multiple_of(me * cols, cols), cols)]
    for copy in copies:
        copy.wait_send()


def tp_order(count, pieces):
    if pieces == 1:
        return [0]
    me = lax.axis_index("tp")
    far = lax.rem(me + 2, 4)
    flip = lambda index: index + 1 - 2 * lax.rem(index, 2)
    return [me, far, flip(me), flip(far)]


def gather_projection(projection):
    count = lax.axis_size("tp")
    if count != 4:
        return [lax.all_gather(projection, "tp", axis=0, tiled=True)]
    far = lax.ppermute(projection, "tp", [(i, (i + 2) % 4) for i in range(4)])
    swap = [(i, i ^ 1) for i in range(4)]
    return [
        projection, far, lax.ppermute(projection, "tp", swap), lax.ppermute(far, "tp", swap)
    ]


def project(gated, residual, weights, out_gain, in_gain):
    count = lax.axis_size("tp")
    rows, width = residual.shape
    depth = gated.shape[1]
    return pl.pallas_call(
        functools.partial(project_kernel, count, len(weights), rows // 3),
        out_shape=(
            jax.ShapeDtypeStruct((rows, width), jnp.bfloat16),
            jax.ShapeDtypeStruct((rows, width // count), jnp.bfloat16),
        ),
        in_specs=[VMEM] * 4 + [ANY] * len(weights),
        out_specs=(VMEM, VMEM),
        scratch_shapes=[
            pltpu.VMEM((count, rows, depth), jnp.bfloat16),
            pltpu.VMEM((count * depth, width), jnp.bfloat16),
            pltpu.VMEM((rows, width), jnp.bfloat16),
            pltpu.SemaphoreType.DMA((2, count - 1)),
            pltpu.SemaphoreType.DMA,
        ],
        compiler_params=pltpu.CompilerParams(
            collective_id=1, has_side_effects=True, vmem_limit_bytes=VMEM_BYTES
        ),
        cost_estimate=pl.CostEstimate(
            flops=2 * rows * width * width, bytes_accessed=80 * 10**6, transcendentals=0
        ),
        name="project",
    )(gated, residual, out_gain[None], in_gain[None], *weights)


def line(value, sources, depth, breadth):
    found = []
    for way in (1, -1):
        held = value
        for step in range(1, depth):
            pairs = [
                ((z - way) * breadth + x, z * breadth + x)
                for z in range(depth)
                for x in range(breadth)
                if 0 <= z - way * step < depth
            ]
            held = lax.ppermute(held, "sp", pairs)
            found.append((held, way * step))
    found.sort(key=lambda entry: abs(entry[1]))
    return [(value, 0)] + found


def flip(value, step, depth):
    pairs = [
        (z * 2 + x, z * 2 + 1 - x) for z in range(depth) for x in range(2) if 0 <= z - step < depth
    ]
    return lax.ppermute(value, "sp", pairs)


def gather_weight(value, crossing_first):
    count = lax.axis_size("sp")
    depth = count // 2
    if crossing_first:
        other = lax.ppermute(value, "sp", [(i, i ^ 1) for i in range(count)])
        return [(held, step, 0) for held, step in line(value, None, depth, 2)] + [
            (held, step, 1) for held, step in line(other, None, depth, 2)
        ]
    own = line(value, None, depth, 2)
    return [(held, step, 0) for held, step in own] + [
        (flip(held, step, depth), step, 1) for held, step in own
    ]


def mixer_kernel(count, depth, plan, normed_ref, first_ref, *refs):
    total = len(plan)
    piece_refs = refs[:total]
    (out_ref, gate_w, up_w, down_w, active, to_core, from_core, to_chip, from_chip, weight_sems,
     sems) = refs[total:]
    me = lax.axis_index("tp")
    rows_all = normed_ref.shape[0]
    cols = out_ref.shape[1]
    sp = lax.axis_index("sp")
    row, col = sp // 2, lax.rem(sp, 2)
    whole = (gate_w, up_w, down_w)
    for which in range(3):
        for ref, (kind, piece, step, crossed, offset) in zip(piece_refs, plan):
            if kind != which:
                continue
            if step is None:
                pltpu.make_async_copy(ref, whole[kind], weight_sems.at[kind]).start()
                continue
            column = col if crossed == 0 else 1 - col
            owner = (row - step) * 2 + column
            high, wide = piece

            @pl.when(jnp.logical_and(row - step >= 0, row - step < depth))
            def _():
                if kind < 2:
                    start = pl.multiple_of(owner * high, high)
                    target = whole[kind].at[pl.ds(start, high), :]
                else:
                    start = pl.multiple_of(owner * wide, wide)
                    target = down_w.at[pl.ds(offset, high), pl.ds(start, wide)]
                pltpu.make_async_copy(ref, target, weight_sems.at[kind]).start()

    greet("tp", count)
    for kind in range(2):
        pltpu.make_async_copy(whole[kind], whole[kind], weight_sems.at[kind]).wait()
    tile = rows_all // 3

    def turn(at, unused):
        rows = pl.ds(pl.multiple_of(at * tile, tile), tile)
        left = normed_ref[rows, :]
        gate = jnp.dot(left, gate_w[...], preferred_element_type=jnp.float32)
        up = jnp.dot(left, up_w[...], preferred_element_type=jnp.float32)
        active[rows, :] = (gate / (1.0 + jnp.exp(-gate)) * up).astype(jnp.bfloat16)
        return unused

    lax.fori_loop(0, 3, turn, 0)
    pltpu.make_async_copy(down_w, down_w, weight_sems.at[2]).wait()

    core = lax.rem(me, 2)
    mate = me + 1 - 2 * core
    chips = count // 2

    def term(target):
        start = pl.multiple_of(target * cols, cols)
        return jnp.dot(
            active[...], down_w[:, pl.ds(start, cols)], preferred_element_type=jnp.float32
        )

    def send(source, target, kind, at, peer):
        return pltpu.make_async_remote_copy(
            source.at[at], target.at[at], sems.at[kind, at], sems.at[kind + 1, at],
            device_id={"tp": peer}, device_id_type=MESH,
        )

    copies = []
    for step in range(1, chips):
        away = lax.rem(me + 2 * step, count)
        to_core[step] = term(away + 1 - 2 * core).astype(jnp.bfloat16)
        hop = send(to_core, from_core, 0, step, mate)
        hop.start()
        mine = term(away)
        hop.wait_recv()
        to_chip[step] = (mine + from_core[step].astype(jnp.float32)).astype(jnp.bfloat16)
        far = send(to_chip, from_chip, 2, step, away)
        far.start()
        copies += [hop, far]
    to_core[0] = term(mate).astype(jnp.bfloat16)
    hop = send(to_core, from_core, 0, 0, mate)
    hop.start()
    result = term(me)
    hop.wait_recv()
    result = result + from_core[0].astype(jnp.float32)
    for far in copies[1::2]:
        far.wait_recv()
    for step in range(1, chips):
        result = result + from_chip[step].astype(jnp.float32)
    out_ref[...] = (first_ref[...].astype(jnp.float32) + 0.5 * result).astype(jnp.bfloat16)
    for copy in copies + [hop]:
        copy.wait_send()


def mixer(normed, first, gate_weight, up_weight, down_weight):
    count, ranks = lax.axis_size("tp"), lax.axis_size("sp")
    rows, width = normed.shape
    hidden = gate_weight.shape[1]
    plan, arrays = [], []

    def take(kind, entries, offset=0):
        for held, step, crossed in entries:
            plan.append((kind, held.shape, step, crossed, offset))
            arrays.append(held)

    if ranks == 8:
        half = hidden // 2
        take(0, gather_weight(gate_weight, False))
        take(1, gather_weight(up_weight, False))
        take(2, gather_weight(down_weight[:half], False))
        take(2, gather_weight(down_weight[half:], True), half)
    else:
        take(0, [(lax.all_gather(gate_weight, "sp", axis=0, tiled=True), None, 0)])
        take(1, [(lax.all_gather(up_weight, "sp", axis=0, tiled=True), None, 0)])
        take(2, [(lax.all_gather(down_weight, "sp", axis=1, tiled=True), None, 0)])
    chips, cols = count // 2, width // count
    buffer = pltpu.VMEM((chips, rows, cols), jnp.bfloat16)
    return pl.pallas_call(
        functools.partial(mixer_kernel, count, ranks // 2, tuple(plan)),
        out_shape=jax.ShapeDtypeStruct((rows, cols), jnp.bfloat16),
        in_specs=[VMEM] * 2 + [ANY] * len(arrays),
        out_specs=VMEM,
        scratch_shapes=[
            pltpu.VMEM((width, hidden), jnp.bfloat16),
            pltpu.VMEM((width, hidden), jnp.bfloat16),
            pltpu.VMEM((hidden, width), jnp.bfloat16),
            pltpu.VMEM((rows, hidden), jnp.bfloat16),
            buffer, buffer, buffer, buffer,
            pltpu.SemaphoreType.DMA((3,)),
            pltpu.SemaphoreType.DMA((4, chips)),
        ],
        compiler_params=pltpu.CompilerParams(
            collective_id=2, has_side_effects=True, vmem_limit_bytes=VMEM_BYTES
        ),
        cost_estimate=pl.CostEstimate(
            flops=6 * rows * width * hidden, bytes_accessed=80 * 10**6, transcendentals=0
        ),
        name="mixer",
    )(normed, first, *arrays)


def body(
    residual,
    query_matrix,
    key_matrix,
    value_matrix,
    output_gate_logit,
    input_gate_log,
    forget_gate_logit,
    extra_head_decay,
    head_norm_gain,
    projection,
    cell_output_gain,
    mixer_input_gain,
    mixer_gate_weight,
    mixer_up_weight,
    mixer_down_weight,
):
    tok_rows = residual.shape[0]
    width = residual.shape[1]
    heads_here = input_gate_log.shape[1]
    query_low = heads_first(query_matrix, heads_here, DQK)
    key_low = heads_first(key_matrix, heads_here, DQK)
    value_low = heads_first(value_matrix, heads_here, DV)
    keyed = key_low.astype(jnp.float32)
    valued = value_low.astype(jnp.float32)
    in_logs = input_gate_log.T
    running_log_total = jnp.cumsum(
        (jax.nn.log_sigmoid(forget_gate_logit) + extra_head_decay).T, axis=-1
    )
    zero_memory = jnp.zeros((heads_here, DV, DQK), jnp.float32)
    zero_normalizer = jnp.zeros((heads_here, DQK), jnp.float32)
    lowest = jnp.full((heads_here,), LOWEST_LOG, jnp.float32)
    local_memory, local_normalizer, local_max = fold_state(
        keyed, valued, in_logs, running_log_total, zero_memory, zero_normalizer, lowest
    )
    prior_decay, prior_memory, prior_normalizer, prior_max = prior_states(
        running_log_total[:, -1], local_memory, local_normalizer, local_max
    )
    start_max = jnp.maximum(prior_decay, prior_max)
    lift = jnp.exp(prior_max - start_max)
    cells = read_out(
        query_low,
        key_low,
        value_low,
        in_logs,
        running_log_total,
        lift[:, None, None] * prior_memory,
        lift[:, None] * prior_normalizer,
        start_max,
    )
    centered = cells - jnp.mean(cells, axis=-1, keepdims=True)
    normed = centered * lax.rsqrt(jnp.mean(centered * centered, axis=-1, keepdims=True) + EPSILON)
    normed = normed * head_norm_gain.reshape(heads_here, DV)[:, None, :]
    normed = normed.transpose(1, 0, 2).reshape(tok_rows, heads_here * DV)
    gated = (normed * jax.nn.sigmoid(output_gate_logit.astype(jnp.float32))).astype(jnp.bfloat16)
    weights = gather_projection(projection)
    normed_rows, own_first = project(gated, residual, weights, cell_output_gain, mixer_input_gain)
    return mixer(normed_rows, own_first, mixer_gate_weight, mixer_up_weight, mixer_down_weight)


def solution(mesh):
    return jax.shard_map(
        body,
        mesh=mesh,
        in_specs=(
            P("sp", None),
            P("sp", "tp"),
            P("sp", "tp"),
            P("sp", "tp"),
            P("sp", "tp"),
            P("sp", "tp"),
            P("sp", "tp"),
            P("sp", "tp"),
            P("tp"),
            P("tp", None),
            P(),
            P(),
            P("sp", "tp"),
            P("sp", "tp"),
            P("tp", "sp"),
        ),
        out_specs=P("sp", "tp"),
        check_vma=False,
    )
```

```python
import functools

import jax
import jax.numpy as jnp
from jax import lax
from jax.experimental import pallas as pl
from jax.experimental.pallas import tpu as pltpu
from jax.sharding import PartitionSpec as P

DQK = 128
DV = 256
MESH = pl.DeviceIdType.MESH
VMEM = pl.BlockSpec(memory_space=pltpu.VMEM)
ANY = pl.BlockSpec(memory_space=pl.ANY)
VMEM_BYTES = 62 * 1024 * 1024

HIGHEST = lax.Precision.HIGHEST
EPSILON = 1e-06
LOWEST_LOG = -1e30


def heads_first(array, heads, width):
    return array.reshape(array.shape[0], heads, width).transpose(1, 0, 2)


def fold_state(keyed, valued, in_logs, running_log_total, memory, normalizer, stabilizer):
    last = running_log_total[:, -1]
    lifted = last[:, None] - running_log_total + in_logs
    new_max = jnp.maximum(last + stabilizer, jnp.max(lifted, axis=-1))
    weights = jnp.exp(lifted - new_max[:, None])
    retained = jnp.exp(last + stabilizer - new_max)
    memory = retained[:, None, None] * memory + jnp.einsum(
        "hsv,hsd->hvd", weights[:, :, None] * valued, keyed, precision=HIGHEST
    )
    normalizer = retained[:, None] * normalizer + jnp.einsum(
        "hs,hsd->hd", weights, keyed, precision=HIGHEST
    )
    return (memory, normalizer, new_max)


def copy_to(source, target, sems, slot, peer):
    return pltpu.make_async_remote_copy(
        source, target, sems.at[(0, *slot)], sems.at[(1, *slot)], device_id=peer, device_id_type=MESH
    )


def layer_kernel(
    ranks, count, heads, carried_by_hand, memory_ref, aux_ref, cum_row, in_row, cum_col, query_ref,
    key_ref, value_ref, ogate_ref, head_gain, residual_ref, out_gain, in_gain, projection_ref,
    gate_ref, up_ref, down_ref, out_ref, slots, aux_slots, memory, aux, gate_w, up_w, down_w,
    weight, gated, blocks, normed, first, active, to_core, from_core, to_chip, from_chip,
    state_sems, aux_sems, line_sems, cross_sems, local_sems, proj_sems, gated_sems, sum_sems,
):
    sp, me = lax.axis_index("sp"), lax.axis_index("tp")
    row, col = sp // 2, lax.rem(sp, 2)
    depth = ranks // 2
    core = lax.rem(me, 2)
    mate = me + 1 - 2 * core
    chips = count // 2
    rows_all, width = residual_ref.shape
    cols = out_ref.shape[1]
    inner = value_ref.shape[1]
    pending = []

    barrier = pltpu.get_barrier_semaphore()
    for axis, size, at in (("sp", ranks, sp), ("tp", count, me)):
        for step in range(1, size):
            pl.semaphore_signal(
                barrier, inc=1, device_id={axis: lax.rem(at + step, size)}, device_id_type=MESH
            )
    pl.semaphore_wait(barrier, ranks + count - 2)

    def when(condition, action):
        pl.when(condition)(action)

    def state_copies(step):
        peer = {"sp": lax.rem(sp + step, ranks)}
        return (
            copy_to(memory_ref, slots.at[step - 1], state_sems, (step - 1,), peer),
            copy_to(aux_ref, aux_slots.at[step - 1], aux_sems, (step - 1,), peer),
        )

    for step in range(1, ranks):

        @pl.when(sp + step < ranks)
        def _():
            for copy in state_copies(step):
                copy.start()

    half = down_w.shape[1] // 2
    high = gate_ref.shape[0]

    def views(kind, owner):
        rows = pl.ds(pl.multiple_of(owner * high, high), high)
        if kind == 0:
            return gate_ref, gate_w.at[rows, :]
        if kind == 1:
            return up_ref, up_w.at[rows, :]
        rows = pl.ds(0 if kind == 2 else half, half)
        return down_ref.at[rows, :], down_w.at[owner, rows, :]

    other = 1 - col
    line_slot = lambda way: 1 if way > 0 else 0

    def along(kind, step, column, mine, way):
        owner = (row - step) * 2 + column
        source, target = views(kind, owner)
        if step != 0 or not mine:
            source = target
        slot = (kind, 0 if mine else 1, abs(step), line_slot(way))
        return copy_to(source, target, line_sems, slot, {"sp": sp + 2 * way})

    def across(kind, step):
        owner = (row - step) * 2 + col
        source, target = views(kind, owner)
        if step != 0:
            source = target
        slot = (kind, step + depth - 1)
        return copy_to(source, target, cross_sems, slot, {"sp": row * 2 + other})

    def crossed(kind, step):
        owner = (row - step) * 2 + other
        source, target = views(kind, owner)
        return copy_to(target, target, cross_sems, (kind, step + depth - 1), {"sp": row * 2 + other})

    def came(kind, step, column, mine):
        owner = (row - step) * 2 + column
        source, target = views(kind, owner)
        way = 1 if step > 0 else -1
        slot = (kind, 0 if mine else 1, abs(step) - 1, line_slot(way))
        return copy_to(target, target, line_sems, slot, {"sp": sp})

    def exists(way):
        return jnp.logical_and(row + way >= 0, row + way < depth)

    def send_along(kind, step, column, mine, way):
        def start():
            along(kind, step, column, mine, way).start()

        has = jnp.logical_and(row - step >= 0, row - step < depth)
        when(jnp.logical_and(has, exists(way)), start)
        pending.append((jnp.logical_and(has, exists(way)), along(kind, step, column, mine, way)))

    def send_across(kind, step):
        has = jnp.logical_and(row - step >= 0, row - step < depth)
        when(has, lambda: across(kind, step).start())
        pending.append((has, across(kind, step)))

    def stage(step, kinds):
        for kind in kinds:
            for column, mine in ((col, True), (other, False)):
                if kind < 3 and not mine:
                    continue
                for way in (1, -1):
                    has = jnp.logical_and(row - way * step >= 0, row - way * step < depth)
                    when(has, lambda: came(kind, way * step, column, mine).wait_recv())
                    if step < depth - 1:
                        send_along(kind, way * step, column, mine, way)
                    if kind < 3:
                        send_across(kind, way * step)

    def finish(kinds):
        for kind in kinds:
            steps = range(1 - depth, depth) if kind < 3 else ()
            for step in steps:
                has = jnp.logical_and(row - step >= 0, row - step < depth)
                when(has, lambda: crossed(kind, step).wait_recv())

    def own(kind):
        source, target = views(kind, sp)
        return pltpu.make_async_copy(source, target, local_sems.at[kind])

    def spread(source, whole, sems):
        sent = [copy_to(source, whole.at[me], sems, (0,), {"tp": mate})]
        for step in range(1, chips):
            peer = {"tp": lax.rem(me + 2 * step, count)}
            sent.append(copy_to(source, whole.at[me], sems, (2 * step,), peer))
        for copy in sent:
            copy.start()
        return sent

    def relay(whole, sems):
        sent = []
        for step in range(1, chips):
            owner = lax.rem(me - 2 * step + count, count)
            block = whole.at[owner]
            copy_to(block, block, sems, (2 * step,), {"tp": mate}).wait_recv()
            sent.append(copy_to(block, block, sems, (2 * step - 1,), {"tp": mate}))
            sent[-1].start()
        return sent

    def collect(whole, sems):
        for step in range(chips):
            owner = lax.rem(mate - 2 * step + count, count)
            block = whole.at[owner]
            slot = 0 if step == 0 else 2 * step - 1
            copy_to(block, block, sems, (slot,), {"tp": mate}).wait_recv()

    if carried_by_hand:
        for kind in range(4):
            if kind == 3:
                send_across(3, 0)
            for way in (1, -1):
                send_along(kind, 0, col, True, way)
            if kind < 3:
                send_across(kind, 0)
            own(kind).start()
    else:
        for ref, whole, at in ((gate_ref, gate_w, 0), (up_ref, up_w, 1)):
            pltpu.make_async_copy(ref, whole, local_sems.at[at]).start()
        pltpu.make_async_copy(down_ref, down_w.at[0], local_sems.at[2]).start()
    own_weight = pltpu.make_async_copy(projection_ref, weight.at[me], local_sems.at[4])
    own_weight.start()
    sent = spread(projection_ref, weight, proj_sems)

    memory[...] = jnp.zeros_like(memory)
    aux[...] = jnp.zeros_like(aux)
    aux[heads : 2 * heads, :] = jnp.full((heads, DQK), LOWEST_LOG, jnp.float32)
    for step in range(ranks - 1, 0, -1):

        @pl.when(sp >= step)
        def _():
            for copy in state_copies(step):
                copy.wait_recv()
            late = aux_slots[step - 1]
            for head in range(heads):
                rows = pl.ds(head * DV, DV)
                early_max = aux[heads + head : heads + head + 1, :]
                late_max = late[heads + head : heads + head + 1, :]
                late_decay = late[2 * heads + head : 2 * heads + head + 1, :]
                joined = jnp.maximum(late_decay + early_max, late_max)
                before = jnp.exp(late_decay + early_max - joined)
                after = jnp.exp(late_max - joined)
                memory[rows, :] = before * memory[rows, :] + after * slots[
                    step - 1, rows, :
                ].astype(jnp.float32)
                aux[head : head + 1, :] = (
                    before * aux[head : head + 1, :] + after * late[head : head + 1, :]
                )
                aux[heads + head : heads + head + 1, :] = joined
                aux[2 * heads + head : 2 * heads + head + 1, :] = (
                    aux[2 * heads + head : 2 * heads + head + 1, :] + late_decay
                )

    if carried_by_hand:
        crossed(3, 0).wait_recv()
        for way in (1, -1):
            send_along(3, 0, other, False, way)
        stage(1, (0,))

    tile = rows_all // 3
    for head in range(heads):
        prior_max = aux[heads + head : heads + head + 1, :]
        start_max = jnp.maximum(aux[2 * heads + head : 2 * heads + head + 1, :], prior_max)
        lift = jnp.exp(prior_max - start_max) * DQK ** (-0.5)
        memory[head * DV : (head + 1) * DV, :] = memory[head * DV : (head + 1) * DV, :] * lift
        aux[head : head + 1, :] = aux[head : head + 1, :] * lift
        aux[2 * heads + head : 2 * heads + head + 1, :] = start_max

    def read(at, unused):
        start = pl.multiple_of(at * tile, tile)
        rows = pl.ds(start, tile)
        causal = start + lax.broadcasted_iota(
            jnp.int32, (tile, rows_all), 0
        ) >= lax.broadcasted_iota(jnp.int32, (tile, rows_all), 1)
        for head in range(heads):
            keys = slice(head * DQK, (head + 1) * DQK)
            values = slice(head * DV, (head + 1) * DV)
            query = query_ref[rows, keys]
            total = cum_col[rows, head : head + 1]
            spread_log = total - cum_row[head : head + 1, :] + in_row[head : head + 1, :]
            spread_log = jnp.where(causal, spread_log, -jnp.inf)
            carried = total + aux[2 * heads + head : 2 * heads + head + 1, :1]
            running = jnp.maximum(carried, jnp.max(spread_log, axis=-1, keepdims=True))
            scores = lax.dot_general(
                query, key_ref[:, keys], (((1,), (1,)), ((), ())),
                preferred_element_type=jnp.float32,
            ) * DQK ** (-0.5)
            weights = jnp.exp(spread_log - running) * scores
            scaled = jnp.exp(carried - running)
            wide = query.astype(jnp.float32)
            numerator = jnp.dot(
                weights.astype(jnp.bfloat16), value_ref[:, values],
                preferred_element_type=jnp.float32,
            ) + scaled * lax.dot_general(
                wide, memory[values, :], (((1,), (1,)), ((), ())), precision=HIGHEST,
                preferred_element_type=jnp.float32,
            )
            denominator = jnp.sum(weights, axis=-1, keepdims=True) + scaled * jnp.sum(
                wide * aux[head : head + 1, :], axis=-1, keepdims=True
            )
            cell = numerator / jnp.maximum(jnp.abs(denominator), jnp.exp(-running))
            centered = cell - jnp.mean(cell, axis=-1, keepdims=True)
            cell = centered * lax.rsqrt(
                jnp.mean(centered * centered, axis=-1, keepdims=True) + EPSILON
            )
            cell = cell * head_gain[:, values]
            gate = ogate_ref[rows, values].astype(jnp.float32)
            gated[rows, values] = (cell * jax.nn.sigmoid(gate)).astype(jnp.bfloat16)
        return unused

    lax.fori_loop(0, 3, read, 0)
    sent += spread(gated, blocks, gated_sems)
    blocks[me] = gated[...]
    if carried_by_hand:
        stage(1, (1, 2, 3))
    sent += relay(weight, proj_sems)
    if carried_by_hand:
        stage(2, (0, 1))
    sent += relay(blocks, gated_sems)
    collect(weight, proj_sems)
    own_weight.wait()
    collect(blocks, gated_sems)

    def turn(at, unused):
        rows = pl.ds(pl.multiple_of(at * tile, tile), tile)
        mixed = jnp.zeros((tile, width), jnp.float32)
        for block in range(count):
            mixed = mixed + jnp.dot(
                blocks[block, rows, :], weight[block], preferred_element_type=jnp.float32
            )
        scale = lax.rsqrt(jnp.mean(mixed * mixed, axis=-1, keepdims=True) + EPSILON)
        total = residual_ref[rows, :].astype(jnp.float32) + mixed * scale * out_gain[...]
        total = total.astype(jnp.bfloat16)
        first[rows, :] = total
        wide = total.astype(jnp.float32)
        scale = lax.rsqrt(jnp.mean(wide * wide, axis=-1, keepdims=True) + EPSILON)
        normed[rows, :] = (wide * scale * in_gain[...]).astype(jnp.bfloat16)
        return unused

    lax.fori_loop(0, 3, turn, 0)

    if carried_by_hand:
        stage(2, (2, 3))
        stage(3, (0, 1))
        finish((0, 1))
        own(0).wait()
        own(1).wait()
    else:
        for ref, whole, at in ((gate_ref, gate_w, 0), (up_ref, up_w, 1)):
            pltpu.make_async_copy(ref, whole, local_sems.at[at]).wait()

    def mix(at, unused):
        rows = pl.ds(pl.multiple_of(at * tile, tile), tile)
        left = normed[rows, :]
        gate = jnp.dot(left, gate_w[...], preferred_element_type=jnp.float32)
        up = jnp.dot(left, up_w[...], preferred_element_type=jnp.float32)
        active[rows, :] = (gate / (1.0 + jnp.exp(-gate)) * up).astype(jnp.bfloat16)
        return unused

    if carried_by_hand:
        stage(3, (2, 3))
    lax.fori_loop(0, 3, mix, 0)
    if carried_by_hand:
        finish((2, 3))
        own(2).wait()
        own(3).wait()
    else:
        pltpu.make_async_copy(down_ref, down_w.at[0], local_sems.at[2]).wait()

    def term(target):
        if carried_by_hand:
            each = cols // down_w.shape[2]
            return jnp.concatenate(
                [
                    jnp.dot(active[...], down_w[target * each + at],
                            preferred_element_type=jnp.float32)
                    for at in range(each)
                ],
                axis=1,
            )
        start = pl.multiple_of(target * cols, cols)
        return jnp.dot(
            active[...], down_w[0, :, pl.ds(start, cols)], preferred_element_type=jnp.float32
        )

    def send(source, target, kind, at, peer):
        return copy_to(source.at[at], target.at[at], sum_sems.at[kind], (at,), {"tp": peer})

    copies = []
    for step in range(1, chips):
        away = lax.rem(me + 2 * step, count)
        to_core[step] = term(away + 1 - 2 * core).astype(jnp.bfloat16)
        hop = send(to_core, from_core, 0, step, mate)
        hop.start()
        mine = term(away)
        hop.wait_recv()
        to_chip[step] = (mine + from_core[step].astype(jnp.float32)).astype(jnp.bfloat16)
        far = send(to_chip, from_chip, 1, step, away)
        far.start()
        copies += [hop, far]
    to_core[0] = term(mate).astype(jnp.bfloat16)
    hop = send(to_core, from_core, 0, 0, mate)
    hop.start()
    result = term(me)
    hop.wait_recv()
    result = result + from_core[0].astype(jnp.float32)
    for far in copies[1::2]:
        far.wait_recv()
    for step in range(1, chips):
        result = result + from_chip[step].astype(jnp.float32)
    own_first = first[:, pl.ds(pl.multiple_of(me * cols, cols), cols)]
    out_ref[...] = (own_first.astype(jnp.float32) + 0.5 * result).astype(jnp.bfloat16)
    for copy in copies + [hop] + sent:
        copy.wait_send()
    for condition, copy in pending:
        when(condition, copy.wait_send)
    for step in range(1, ranks):

        @pl.when(sp + step < ranks)
        def _():
            for copy in state_copies(step):
                copy.wait_send()


def layer(states, logs, cell_inputs, residual, gains, weights):
    decay, memory, normalizer, maximum = states
    running_log_total, in_logs = logs
    ranks, count = lax.axis_size("sp"), lax.axis_size("tp")
    heads = decay.shape[0]
    rows, width = residual.shape
    projection, gate_weight, up_weight, down_weight = weights
    hidden = gate_weight.shape[1]
    inner = projection.shape[0]
    carried_by_hand = ranks == 8
    if carried_by_hand:
        down_shape = (ranks, hidden, down_weight.shape[1])
    else:
        gate_weight = lax.all_gather(gate_weight, "sp", axis=0, tiled=True)
        up_weight = lax.all_gather(up_weight, "sp", axis=0, tiled=True)
        down_weight = lax.all_gather(down_weight, "sp", axis=1, tiled=True)
        down_shape = (1, hidden, width)
    fill = lambda row: jnp.broadcast_to(row[:, None], (heads, DQK))
    aux = jnp.concatenate([normalizer, fill(maximum), fill(decay)])
    height = -(-3 * heads // 8) * 8
    aux = jnp.pad(aux, ((0, height - 3 * heads), (0, 0)))
    low = memory.reshape(heads * DV, DQK).astype(jnp.bfloat16)
    chips, cols, depth = count // 2, width // count, ranks // 2
    buffer = pltpu.VMEM((chips, rows, cols), jnp.bfloat16)
    dma = pltpu.SemaphoreType.DMA
    return pl.pallas_call(
        functools.partial(layer_kernel, ranks, count, heads, carried_by_hand),
        out_shape=jax.ShapeDtypeStruct((rows, cols), jnp.bfloat16),
        in_specs=[VMEM] * 13 + [ANY] * 4,
        out_specs=VMEM,
        scratch_shapes=[
            pltpu.VMEM((ranks - 1, heads * DV, DQK), jnp.bfloat16),
            pltpu.VMEM((ranks - 1, height, DQK), jnp.float32),
            pltpu.VMEM((heads * DV, DQK), jnp.float32),
            pltpu.VMEM((height, DQK), jnp.float32),
            pltpu.VMEM((width, hidden), jnp.bfloat16),
            pltpu.VMEM((width, hidden), jnp.bfloat16),
            pltpu.VMEM(down_shape, jnp.bfloat16),
            pltpu.VMEM((count, inner, width), jnp.bfloat16),
            pltpu.VMEM((rows, inner), jnp.bfloat16),
            pltpu.VMEM((count, rows, inner), jnp.bfloat16),
            pltpu.VMEM((rows, width), jnp.bfloat16),
            pltpu.VMEM((rows, width), jnp.bfloat16),
            pltpu.VMEM((rows, hidden), jnp.bfloat16),
            buffer, buffer, buffer, buffer,
            dma((2, ranks - 1)),
            dma((2, ranks - 1)),
            dma((2, 4, 2, depth, 2)),
            dma((2, 4, 2 * depth - 1)),
            dma((5,)),
            dma((2, count)),
            dma((2, count)),
            dma((2, 2, chips)),
        ],
        compiler_params=pltpu.CompilerParams(
            collective_id=0, has_side_effects=True, vmem_limit_bytes=VMEM_BYTES
        ),
        name="layer",
    )(
        low, aux, running_log_total, in_logs, running_log_total.T, *cell_inputs, residual,
        *gains, projection, gate_weight, up_weight, down_weight,
    )


def body(
    residual,
    query_matrix,
    key_matrix,
    value_matrix,
    output_gate_logit,
    input_gate_log,
    forget_gate_logit,
    extra_head_decay,
    head_norm_gain,
    projection,
    cell_output_gain,
    mixer_input_gain,
    mixer_gate_weight,
    mixer_up_weight,
    mixer_down_weight,
):
    heads_here = input_gate_log.shape[1]
    key_low = heads_first(key_matrix, heads_here, DQK)
    value_low = heads_first(value_matrix, heads_here, DV)
    keyed = key_low.astype(jnp.float32)
    valued = value_low.astype(jnp.float32)
    in_logs = input_gate_log.T
    running_log_total = jnp.cumsum(
        (jax.nn.log_sigmoid(forget_gate_logit) + extra_head_decay).T, axis=-1
    )
    zero_memory = jnp.zeros((heads_here, DV, DQK), jnp.float32)
    zero_normalizer = jnp.zeros((heads_here, DQK), jnp.float32)
    lowest = jnp.full((heads_here,), LOWEST_LOG, jnp.float32)
    local_memory, local_normalizer, local_max = fold_state(
        keyed, valued, in_logs, running_log_total, zero_memory, zero_normalizer, lowest
    )
    return layer(
        (running_log_total[:, -1], local_memory, local_normalizer, local_max),
        (running_log_total, in_logs),
        (query_matrix, key_matrix, value_matrix, output_gate_logit, head_norm_gain[None]),
        residual,
        (cell_output_gain[None], mixer_input_gain[None]),
        (projection, mixer_gate_weight, mixer_up_weight, mixer_down_weight),
    )


def solution(mesh):
    return jax.shard_map(
        body,
        mesh=mesh,
        in_specs=(
            P("sp", None),
            P("sp", "tp"),
            P("sp", "tp"),
            P("sp", "tp"),
            P("sp", "tp"),
            P("sp", "tp"),
            P("sp", "tp"),
            P("sp", "tp"),
            P("tp"),
            P("tp", None),
            P(),
            P(),
            P("sp", "tp"),
            P("sp", "tp"),
            P("tp", "sp"),
        ),
        out_specs=P("sp", "tp"),
        check_vma=False,
    )
```

```python
import functools

import jax
import jax.numpy as jnp
from jax import lax
from jax.experimental import pallas as pl
from jax.experimental.pallas import tpu as pltpu
from jax.sharding import PartitionSpec as P

DQK = 128
DV = 256
MESH = pl.DeviceIdType.MESH
VMEM = pl.BlockSpec(memory_space=pltpu.VMEM)
ANY = pl.BlockSpec(memory_space=pl.ANY)
VMEM_BYTES = 62 * 1024 * 1024

HIGHEST = lax.Precision.HIGHEST
EPSILON = 1e-06
LOWEST_LOG = -1e30


def heads_first(array, heads, width):
    return array.reshape(array.shape[0], heads, width).transpose(1, 0, 2)


def fold_state(keyed, valued, in_logs, running_log_total, memory, normalizer, stabilizer):
    last = running_log_total[:, -1]
    lifted = last[:, None] - running_log_total + in_logs
    new_max = jnp.maximum(last + stabilizer, jnp.max(lifted, axis=-1))
    weights = jnp.exp(lifted - new_max[:, None])
    retained = jnp.exp(last + stabilizer - new_max)
    memory = retained[:, None, None] * memory + jnp.einsum(
        "hsv,hsd->hvd", weights[:, :, None] * valued, keyed, precision=HIGHEST
    )
    normalizer = retained[:, None] * normalizer + jnp.einsum(
        "hs,hsd->hd", weights, keyed, precision=HIGHEST
    )
    return (memory, normalizer, new_max)


def copy_to(source, target, sems, slot, peer):
    return pltpu.make_async_remote_copy(
        source, target, sems.at[(0, *slot)], sems.at[(1, *slot)], device_id=peer, device_id_type=MESH
    )


def layer_kernel(
    ranks, count, heads, carried_by_hand, memory_ref, aux_ref, cum_row, in_row, cum_col, query_ref,
    key_ref, value_ref, ogate_ref, head_gain, residual_ref, out_gain, in_gain, projection_ref,
    gate_ref, up_ref, down_ref, out_ref, slots, aux_slots, memory, aux, gate_w, up_w, down_w,
    weight, gated, blocks, normed, first, active, to_core, from_core, to_chip, from_chip,
    state_sems, aux_sems, line_sems, cross_sems, local_sems, proj_sems, gated_sems, sum_sems,
):
    sp, me = lax.axis_index("sp"), lax.axis_index("tp")
    row, col = sp // 2, lax.rem(sp, 2)
    depth = ranks // 2
    core = lax.rem(me, 2)
    mate = me + 1 - 2 * core
    chips = count // 2
    rows_all, width = residual_ref.shape
    cols = out_ref.shape[1]
    inner = value_ref.shape[1]
    pending = []

    barrier = pltpu.get_barrier_semaphore()
    for axis, size, at in (("sp", ranks, sp), ("tp", count, me)):
        for step in range(1, size):
            pl.semaphore_signal(
                barrier, inc=1, device_id={axis: lax.rem(at + step, size)}, device_id_type=MESH
            )
    pl.semaphore_wait(barrier, ranks + count - 2)

    def when(condition, action):
        pl.when(condition)(action)

    def state_copies(step):
        peer = {"sp": lax.rem(sp + step, ranks)}
        return (
            copy_to(memory_ref, slots.at[step - 1], state_sems, (step - 1,), peer),
            copy_to(aux_ref, aux_slots.at[step - 1], aux_sems, (step - 1,), peer),
        )

    for step in range(1, ranks):

        @pl.when(sp + step < ranks)
        def _():
            for copy in state_copies(step):
                copy.start()

    half = down_w.shape[1] // 2
    high = gate_ref.shape[0]

    def views(kind, owner):
        rows = pl.ds(pl.multiple_of(owner * high, high), high)
        if kind == 0:
            return gate_ref, gate_w.at[rows, :]
        if kind == 1:
            return up_ref, up_w.at[rows, :]
        rows = pl.ds(0 if kind == 2 else half, half)
        return down_ref.at[rows, :], down_w.at[owner, rows, :]

    other = 1 - col
    line_slot = lambda way: 1 if way > 0 else 0

    def along(kind, step, column, mine, way):
        owner = (row - step) * 2 + column
        source, target = views(kind, owner)
        if step != 0 or not mine:
            source = target
        slot = (kind, 0 if mine else 1, abs(step), line_slot(way))
        return copy_to(source, target, line_sems, slot, {"sp": sp + 2 * way})

    def across(kind, step):
        owner = (row - step) * 2 + col
        source, target = views(kind, owner)
        if step != 0:
            source = target
        slot = (kind, step + depth - 1)
        return copy_to(source, target, cross_sems, slot, {"sp": row * 2 + other})

    def crossed(kind, step):
        owner = (row - step) * 2 + other
        source, target = views(kind, owner)
        return copy_to(target, target, cross_sems, (kind, step + depth - 1), {"sp": row * 2 + other})

    def came(kind, step, column, mine):
        owner = (row - step) * 2 + column
        source, target = views(kind, owner)
        way = 1 if step > 0 else -1
        slot = (kind, 0 if mine else 1, abs(step) - 1, line_slot(way))
        return copy_to(target, target, line_sems, slot, {"sp": sp})

    def exists(way):
        return jnp.logical_and(row + way >= 0, row + way < depth)

    def send_along(kind, step, column, mine, way):
        def start():
            along(kind, step, column, mine, way).start()

        has = jnp.logical_and(row - step >= 0, row - step < depth)
        when(jnp.logical_and(has, exists(way)), start)
        pending.append((jnp.logical_and(has, exists(way)), along(kind, step, column, mine, way)))

    def send_across(kind, step):
        has = jnp.logical_and(row - step >= 0, row - step < depth)
        when(has, lambda: across(kind, step).start())
        pending.append((has, across(kind, step)))

    def stage(step, kinds):
        for kind in kinds:
            for column, mine in ((col, True), (other, False)):
                if kind < 3 and not mine:
                    continue
                for way in (1, -1):
                    has = jnp.logical_and(row - way * step >= 0, row - way * step < depth)
                    when(has, lambda: came(kind, way * step, column, mine).wait_recv())
                    if step < depth - 1:
                        send_along(kind, way * step, column, mine, way)
                    if kind < 3:
                        send_across(kind, way * step)

    def finish(kinds):
        for kind in kinds:
            steps = range(1 - depth, depth) if kind < 3 else ()
            for step in steps:
                has = jnp.logical_and(row - step >= 0, row - step < depth)
                when(has, lambda: crossed(kind, step).wait_recv())

    def own(kind):
        source, target = views(kind, sp)
        return pltpu.make_async_copy(source, target, local_sems.at[kind])

    def spread(source, whole, sems):
        sent = [copy_to(source, whole.at[me], sems, (0,), {"tp": mate})]
        for step in range(1, chips):
            peer = {"tp": lax.rem(me + 2 * step, count)}
            sent.append(copy_to(source, whole.at[me], sems, (2 * step,), peer))
        for copy in sent:
            copy.start()
        return sent

    def relay(whole, sems):
        sent = []
        for step in range(1, chips):
            owner = lax.rem(me - 2 * step + count, count)
            block = whole.at[owner]
            copy_to(block, block, sems, (2 * step,), {"tp": mate}).wait_recv()
            sent.append(copy_to(block, block, sems, (2 * step - 1,), {"tp": mate}))
            sent[-1].start()
        return sent

    def collect(whole, sems):
        for step in range(chips):
            owner = lax.rem(mate - 2 * step + count, count)
            block = whole.at[owner]
            slot = 0 if step == 0 else 2 * step - 1
            copy_to(block, block, sems, (slot,), {"tp": mate}).wait_recv()

    if carried_by_hand:
        for kind in range(4):
            if kind == 3:
                send_across(3, 0)
            for way in (1, -1):
                send_along(kind, 0, col, True, way)
            if kind < 3:
                send_across(kind, 0)
            own(kind).start()
    else:
        for ref, whole, at in ((gate_ref, gate_w, 0), (up_ref, up_w, 1)):
            pltpu.make_async_copy(ref, whole, local_sems.at[at]).start()
        pltpu.make_async_copy(down_ref, down_w.at[0], local_sems.at[2]).start()
    own_weight = pltpu.make_async_copy(projection_ref, weight.at[me], local_sems.at[4])
    own_weight.start()
    sent = spread(projection_ref, weight, proj_sems)

    memory[...] = jnp.zeros_like(memory)
    aux[...] = jnp.zeros_like(aux)
    aux[heads : 2 * heads, :] = jnp.full((heads, DQK), LOWEST_LOG, jnp.float32)
    for step in range(ranks - 1, 0, -1):

        @pl.when(sp >= step)
        def _():
            for copy in state_copies(step):
                copy.wait_recv()
            late = aux_slots[step - 1]
            for head in range(heads):
                rows = pl.ds(head * DV, DV)
                early_max = aux[heads + head : heads + head + 1, :]
                late_max = late[heads + head : heads + head + 1, :]
                late_decay = late[2 * heads + head : 2 * heads + head + 1, :]
                joined = jnp.maximum(late_decay + early_max, late_max)
                before = jnp.exp(late_decay + early_max - joined)
                after = jnp.exp(late_max - joined)
                memory[rows, :] = before * memory[rows, :] + after * slots[
                    step - 1, rows, :
                ].astype(jnp.float32)
                aux[head : head + 1, :] = (
                    before * aux[head : head + 1, :] + after * late[head : head + 1, :]
                )
                aux[heads + head : heads + head + 1, :] = joined
                aux[2 * heads + head : 2 * heads + head + 1, :] = (
                    aux[2 * heads + head : 2 * heads + head + 1, :] + late_decay
                )

    if carried_by_hand:
        stage(1, (0,))

    tile = rows_all // 3
    for head in range(heads):
        prior_max = aux[heads + head : heads + head + 1, :]
        start_max = jnp.maximum(aux[2 * heads + head : 2 * heads + head + 1, :], prior_max)
        lift = jnp.exp(prior_max - start_max) * DQK ** (-0.5)
        memory[head * DV : (head + 1) * DV, :] = memory[head * DV : (head + 1) * DV, :] * lift
        aux[head : head + 1, :] = aux[head : head + 1, :] * lift
        aux[2 * heads + head : 2 * heads + head + 1, :] = start_max

    def read(at, unused):
        start = pl.multiple_of(at * tile, tile)
        rows = pl.ds(start, tile)
        causal = start + lax.broadcasted_iota(
            jnp.int32, (tile, rows_all), 0
        ) >= lax.broadcasted_iota(jnp.int32, (tile, rows_all), 1)
        for head in range(heads):
            keys = slice(head * DQK, (head + 1) * DQK)
            values = slice(head * DV, (head + 1) * DV)
            query = query_ref[rows, keys]
            total = cum_col[rows, head : head + 1]
            spread_log = total - cum_row[head : head + 1, :] + in_row[head : head + 1, :]
            spread_log = jnp.where(causal, spread_log, -jnp.inf)
            carried = total + aux[2 * heads + head : 2 * heads + head + 1, :1]
            running = jnp.maximum(carried, jnp.max(spread_log, axis=-1, keepdims=True))
            scores = lax.dot_general(
                query, key_ref[:, keys], (((1,), (1,)), ((), ())),
                preferred_element_type=jnp.float32,
            ) * DQK ** (-0.5)
            weights = jnp.exp(spread_log - running) * scores
            scaled = jnp.exp(carried - running)
            wide = query.astype(jnp.float32)
            numerator = jnp.dot(
                weights.astype(jnp.bfloat16), value_ref[:, values],
                preferred_element_type=jnp.float32,
            ) + scaled * lax.dot_general(
                wide, memory[values, :], (((1,), (1,)), ((), ())), precision=HIGHEST,
                preferred_element_type=jnp.float32,
            )
            denominator = jnp.sum(weights, axis=-1, keepdims=True) + scaled * jnp.sum(
                wide * aux[head : head + 1, :], axis=-1, keepdims=True
            )
            cell = numerator / jnp.maximum(jnp.abs(denominator), jnp.exp(-running))
            centered = cell - jnp.mean(cell, axis=-1, keepdims=True)
            cell = centered * lax.rsqrt(
                jnp.mean(centered * centered, axis=-1, keepdims=True) + EPSILON
            )
            cell = cell * head_gain[:, values]
            gate = ogate_ref[rows, values].astype(jnp.float32)
            gated[rows, values] = (cell * jax.nn.sigmoid(gate)).astype(jnp.bfloat16)
        return unused

    lax.fori_loop(0, 3, read, 0)
    sent += spread(gated, blocks, gated_sems)
    blocks[me] = gated[...]
    if carried_by_hand:
        stage(1, (1, 2))
        crossed(3, 0).wait_recv()
        for way in (1, -1):
            send_along(3, 0, other, False, way)
        stage(1, (3,))
    sent += relay(weight, proj_sems)
    if carried_by_hand:
        stage(2, (0, 1))
    sent += relay(blocks, gated_sems)
    collect(weight, proj_sems)
    own_weight.wait()
    collect(blocks, gated_sems)

    def turn(at, unused):
        rows = pl.ds(pl.multiple_of(at * tile, tile), tile)
        mixed = jnp.zeros((tile, width), jnp.float32)
        for block in range(count):
            mixed = mixed + jnp.dot(
                blocks[block, rows, :], weight[block], preferred_element_type=jnp.float32
            )
        scale = lax.rsqrt(jnp.mean(mixed * mixed, axis=-1, keepdims=True) + EPSILON)
        total = residual_ref[rows, :].astype(jnp.float32) + mixed * scale * out_gain[...]
        total = total.astype(jnp.bfloat16)
        first[rows, :] = total
        wide = total.astype(jnp.float32)
        scale = lax.rsqrt(jnp.mean(wide * wide, axis=-1, keepdims=True) + EPSILON)
        normed[rows, :] = (wide * scale * in_gain[...]).astype(jnp.bfloat16)
        return unused

    lax.fori_loop(0, 3, turn, 0)

    if carried_by_hand:
        stage(2, (2, 3))
        stage(3, (0, 1, 2))
        finish((0, 1))
        own(0).wait()
        own(1).wait()
    else:
        for ref, whole, at in ((gate_ref, gate_w, 0), (up_ref, up_w, 1)):
            pltpu.make_async_copy(ref, whole, local_sems.at[at]).wait()

    def mix(at, unused):
        rows = pl.ds(pl.multiple_of(at * tile, tile), tile)
        left = normed[rows, :]
        gate = jnp.dot(left, gate_w[...], preferred_element_type=jnp.float32)
        up = jnp.dot(left, up_w[...], preferred_element_type=jnp.float32)
        active[rows, :] = (gate / (1.0 + jnp.exp(-gate)) * up).astype(jnp.bfloat16)
        return unused

    lax.fori_loop(0, 3, mix, 0)
    if carried_by_hand:
        stage(3, (3,))
        finish((2, 3))
        own(2).wait()
        own(3).wait()
    else:
        pltpu.make_async_copy(down_ref, down_w.at[0], local_sems.at[2]).wait()

    def term(target):
        if carried_by_hand:
            each = cols // down_w.shape[2]
            return jnp.concatenate(
                [
                    jnp.dot(active[...], down_w[target * each + at],
                            preferred_element_type=jnp.float32)
                    for at in range(each)
                ],
                axis=1,
            )
        start = pl.multiple_of(target * cols, cols)
        return jnp.dot(
            active[...], down_w[0, :, pl.ds(start, cols)], preferred_element_type=jnp.float32
        )

    def send(source, target, kind, at, peer):
        return copy_to(source.at[at], target.at[at], sum_sems.at[kind], (at,), {"tp": peer})

    copies = []
    for step in range(1, chips):
        away = lax.rem(me + 2 * step, count)
        to_core[step] = term(away + 1 - 2 * core).astype(jnp.bfloat16)
        hop = send(to_core, from_core, 0, step, mate)
        hop.start()
        mine = term(away)
        hop.wait_recv()
        to_chip[step] = (mine + from_core[step].astype(jnp.float32)).astype(jnp.bfloat16)
        far = send(to_chip, from_chip, 1, step, away)
        far.start()
        copies += [hop, far]
    to_core[0] = term(mate).astype(jnp.bfloat16)
    hop = send(to_core, from_core, 0, 0, mate)
    hop.start()
    result = term(me)
    hop.wait_recv()
    result = result + from_core[0].astype(jnp.float32)
    for far in copies[1::2]:
        far.wait_recv()
    for step in range(1, chips):
        result = result + from_chip[step].astype(jnp.float32)
    own_first = first[:, pl.ds(pl.multiple_of(me * cols, cols), cols)]
    out_ref[...] = (own_first.astype(jnp.float32) + 0.5 * result).astype(jnp.bfloat16)
    for copy in copies + [hop] + sent:
        copy.wait_send()
    for condition, copy in pending:
        when(condition, copy.wait_send)
    for step in range(1, ranks):

        @pl.when(sp + step < ranks)
        def _():
            for copy in state_copies(step):
                copy.wait_send()


def layer(states, logs, cell_inputs, residual, gains, weights):
    decay, memory, normalizer, maximum = states
    running_log_total, in_logs = logs
    ranks, count = lax.axis_size("sp"), lax.axis_size("tp")
    heads = decay.shape[0]
    rows, width = residual.shape
    projection, gate_weight, up_weight, down_weight = weights
    hidden = gate_weight.shape[1]
    inner = projection.shape[0]
    carried_by_hand = ranks == 8
    if carried_by_hand:
        down_shape = (ranks, hidden, down_weight.shape[1])
    else:
        gate_weight = lax.all_gather(gate_weight, "sp", axis=0, tiled=True)
        up_weight = lax.all_gather(up_weight, "sp", axis=0, tiled=True)
        down_weight = lax.all_gather(down_weight, "sp", axis=1, tiled=True)
        down_shape = (1, hidden, width)
    fill = lambda row: jnp.broadcast_to(row[:, None], (heads, DQK))
    aux = jnp.concatenate([normalizer, fill(maximum), fill(decay)])
    height = -(-3 * heads // 8) * 8
    aux = jnp.pad(aux, ((0, height - 3 * heads), (0, 0)))
    low = memory.reshape(heads * DV, DQK).astype(jnp.bfloat16)
    chips, cols, depth = count // 2, width // count, ranks // 2
    buffer = pltpu.VMEM((chips, rows, cols), jnp.bfloat16)
    dma = pltpu.SemaphoreType.DMA
    return pl.pallas_call(
        functools.partial(layer_kernel, ranks, count, heads, carried_by_hand),
        out_shape=jax.ShapeDtypeStruct((rows, cols), jnp.bfloat16),
        in_specs=[VMEM] * 13 + [ANY] * 4,
        out_specs=VMEM,
        scratch_shapes=[
            pltpu.VMEM((ranks - 1, heads * DV, DQK), jnp.bfloat16),
            pltpu.VMEM((ranks - 1, height, DQK), jnp.float32),
            pltpu.VMEM((heads * DV, DQK), jnp.float32),
            pltpu.VMEM((height, DQK), jnp.float32),
            pltpu.VMEM((width, hidden), jnp.bfloat16),
            pltpu.VMEM((width, hidden), jnp.bfloat16),
            pltpu.VMEM(down_shape, jnp.bfloat16),
            pltpu.VMEM((count, inner, width), jnp.bfloat16),
            pltpu.VMEM((rows, inner), jnp.bfloat16),
            pltpu.VMEM((count, rows, inner), jnp.bfloat16),
            pltpu.VMEM((rows, width), jnp.bfloat16),
            pltpu.VMEM((rows, width), jnp.bfloat16),
            pltpu.VMEM((rows, hidden), jnp.bfloat16),
            buffer, buffer, buffer, buffer,
            dma((2, ranks - 1)),
            dma((2, ranks - 1)),
            dma((2, 4, 2, depth, 2)),
            dma((2, 4, 2 * depth - 1)),
            dma((5,)),
            dma((2, count)),
            dma((2, count)),
            dma((2, 2, chips)),
        ],
        compiler_params=pltpu.CompilerParams(
            collective_id=0, has_side_effects=True, vmem_limit_bytes=VMEM_BYTES
        ),
        name="layer",
    )(
        low, aux, running_log_total, in_logs, running_log_total.T, *cell_inputs, residual,
        *gains, projection, gate_weight, up_weight, down_weight,
    )


def body(
    residual,
    query_matrix,
    key_matrix,
    value_matrix,
    output_gate_logit,
    input_gate_log,
    forget_gate_logit,
    extra_head_decay,
    head_norm_gain,
    projection,
    cell_output_gain,
    mixer_input_gain,
    mixer_gate_weight,
    mixer_up_weight,
    mixer_down_weight,
):
    heads_here = input_gate_log.shape[1]
    key_low = heads_first(key_matrix, heads_here, DQK)
    value_low = heads_first(value_matrix, heads_here, DV)
    keyed = key_low.astype(jnp.float32)
    valued = value_low.astype(jnp.float32)
    in_logs = input_gate_log.T
    running_log_total = jnp.cumsum(
        (jax.nn.log_sigmoid(forget_gate_logit) + extra_head_decay).T, axis=-1
    )
    zero_memory = jnp.zeros((heads_here, DV, DQK), jnp.float32)
    zero_normalizer = jnp.zeros((heads_here, DQK), jnp.float32)
    lowest = jnp.full((heads_here,), LOWEST_LOG, jnp.float32)
    local_memory, local_normalizer, local_max = fold_state(
        keyed, valued, in_logs, running_log_total, zero_memory, zero_normalizer, lowest
    )
    return layer(
        (running_log_total[:, -1], local_memory, local_normalizer, local_max),
        (running_log_total, in_logs),
        (query_matrix, key_matrix, value_matrix, output_gate_logit, head_norm_gain[None]),
        residual,
        (cell_output_gain[None], mixer_input_gain[None]),
        (projection, mixer_gate_weight, mixer_up_weight, mixer_down_weight),
    )


def solution(mesh):
    return jax.shard_map(
        body,
        mesh=mesh,
        in_specs=(
            P("sp", None),
            P("sp", "tp"),
            P("sp", "tp"),
            P("sp", "tp"),
            P("sp", "tp"),
            P("sp", "tp"),
            P("sp", "tp"),
            P("sp", "tp"),
            P("tp"),
            P("tp", None),
            P(),
            P(),
            P("sp", "tp"),
            P("sp", "tp"),
            P("tp", "sp"),
        ),
        out_specs=P("sp", "tp"),
        check_vma=False,
    )
```

```python
import functools

import jax
import jax.numpy as jnp
from jax import lax
from jax.experimental import pallas as pl
from jax.experimental.pallas import tpu as pltpu
from jax.sharding import PartitionSpec as P

DQK = 128
DV = 256
MESH = pl.DeviceIdType.MESH
VMEM = pl.BlockSpec(memory_space=pltpu.VMEM)
ANY = pl.BlockSpec(memory_space=pl.ANY)
VMEM_BYTES = 62 * 1024 * 1024

HIGHEST = lax.Precision.HIGHEST
EPSILON = 1e-06
LOWEST_LOG = -1e30


def heads_first(array, heads, width):
    return array.reshape(array.shape[0], heads, width).transpose(1, 0, 2)


def fold_state(keyed, valued, in_logs, running_log_total, memory, normalizer, stabilizer):
    last = running_log_total[:, -1]
    lifted = last[:, None] - running_log_total + in_logs
    new_max = jnp.maximum(last + stabilizer, jnp.max(lifted, axis=-1))
    weights = jnp.exp(lifted - new_max[:, None])
    retained = jnp.exp(last + stabilizer - new_max)
    memory = retained[:, None, None] * memory + jnp.einsum(
        "hsv,hsd->hvd", weights[:, :, None] * valued, keyed, precision=HIGHEST
    )
    normalizer = retained[:, None] * normalizer + jnp.einsum(
        "hs,hsd->hd", weights, keyed, precision=HIGHEST
    )
    return (memory, normalizer, new_max)


def copy_to(source, target, sems, slot, peer):
    return pltpu.make_async_remote_copy(
        source, target, sems.at[(0, *slot)], sems.at[(1, *slot)], device_id=peer, device_id_type=MESH
    )


def layer_kernel(
    ranks, count, heads, carried_by_hand, memory_ref, aux_ref, cum_row, in_row, cum_col, query_ref,
    key_ref, value_ref, ogate_ref, head_gain, residual_ref, out_gain, in_gain, projection_ref,
    gate_ref, up_ref, down_ref, out_ref, slots, aux_slots, memory, aux, gate_w, up_w, down_w,
    weight, gated, blocks, normed, first, active, to_core, from_core, to_chip, from_chip,
    state_sems, aux_sems, line_sems, cross_sems, local_sems, proj_sems, gated_sems, sum_sems,
):
    sp, me = lax.axis_index("sp"), lax.axis_index("tp")
    row, col = sp // 2, lax.rem(sp, 2)
    depth = ranks // 2
    core = lax.rem(me, 2)
    mate = me + 1 - 2 * core
    chips = count // 2
    rows_all, width = residual_ref.shape
    cols = out_ref.shape[1]
    inner = value_ref.shape[1]
    pending = []

    barrier = pltpu.get_barrier_semaphore()
    for axis, size, at in (("sp", ranks, sp), ("tp", count, me)):
        for step in range(1, size):
            pl.semaphore_signal(
                barrier, inc=1, device_id={axis: lax.rem(at + step, size)}, device_id_type=MESH
            )
    pl.semaphore_wait(barrier, ranks + count - 2)

    def when(condition, action):
        pl.when(condition)(action)

    def state_copies(step):
        peer = {"sp": lax.rem(sp + step, ranks)}
        return (
            copy_to(memory_ref, slots.at[step - 1], state_sems, (step - 1,), peer),
            copy_to(aux_ref, aux_slots.at[step - 1], aux_sems, (step - 1,), peer),
        )

    for step in range(1, ranks):

        @pl.when(sp + step < ranks)
        def _():
            for copy in state_copies(step):
                copy.start()

    half = down_w.shape[1] // 2
    high = gate_ref.shape[0]

    def views(kind, owner):
        rows = pl.ds(pl.multiple_of(owner * high, high), high)
        if kind == 0:
            return gate_ref, gate_w.at[rows, :]
        if kind == 1:
            return up_ref, up_w.at[rows, :]
        rows = pl.ds(0 if kind == 2 else half, half)
        return down_ref.at[rows, :], down_w.at[owner, rows, :]

    other = 1 - col
    line_slot = lambda way: 1 if way > 0 else 0

    def along(kind, step, column, mine, way):
        owner = (row - step) * 2 + column
        source, target = views(kind, owner)
        if step != 0 or not mine:
            source = target
        slot = (kind, 0 if mine else 1, abs(step), line_slot(way))
        return copy_to(source, target, line_sems, slot, {"sp": sp + 2 * way})

    def across(kind, step):
        owner = (row - step) * 2 + col
        source, target = views(kind, owner)
        if step != 0:
            source = target
        slot = (kind, step + depth - 1)
        return copy_to(source, target, cross_sems, slot, {"sp": row * 2 + other})

    def crossed(kind, step):
        owner = (row - step) * 2 + other
        source, target = views(kind, owner)
        return copy_to(target, target, cross_sems, (kind, step + depth - 1), {"sp": row * 2 + other})

    def came(kind, step, column, mine):
        owner = (row - step) * 2 + column
        source, target = views(kind, owner)
        way = 1 if step > 0 else -1
        slot = (kind, 0 if mine else 1, abs(step) - 1, line_slot(way))
        return copy_to(target, target, line_sems, slot, {"sp": sp})

    def exists(way):
        return jnp.logical_and(row + way >= 0, row + way < depth)

    def send_along(kind, step, column, mine, way):
        def start():
            along(kind, step, column, mine, way).start()

        has = jnp.logical_and(row - step >= 0, row - step < depth)
        when(jnp.logical_and(has, exists(way)), start)
        pending.append((jnp.logical_and(has, exists(way)), along(kind, step, column, mine, way)))

    def send_across(kind, step):
        has = jnp.logical_and(row - step >= 0, row - step < depth)
        when(has, lambda: across(kind, step).start())
        pending.append((has, across(kind, step)))

    def stage(step, kinds):
        for kind in kinds:
            for column, mine in ((col, True), (other, False)):
                if kind < 3 and not mine:
                    continue
                for way in (1, -1):
                    has = jnp.logical_and(row - way * step >= 0, row - way * step < depth)
                    when(has, lambda: came(kind, way * step, column, mine).wait_recv())
                    if step < depth - 1:
                        send_along(kind, way * step, column, mine, way)
                    if kind < 3:
                        send_across(kind, way * step)

    def finish(kinds):
        for kind in kinds:
            steps = range(1 - depth, depth) if kind < 3 else ()
            for step in steps:
                has = jnp.logical_and(row - step >= 0, row - step < depth)
                when(has, lambda: crossed(kind, step).wait_recv())

    def own(kind):
        source, target = views(kind, sp)
        return pltpu.make_async_copy(source, target, local_sems.at[kind])

    def spread(source, whole, sems):
        sent = [copy_to(source, whole.at[me], sems, (0,), {"tp": mate})]
        for step in range(1, chips):
            peer = {"tp": lax.rem(me + 2 * step, count)}
            sent.append(copy_to(source, whole.at[me], sems, (2 * step,), peer))
        for copy in sent:
            copy.start()
        return sent

    def relay(whole, sems):
        sent = []
        for step in range(1, chips):
            owner = lax.rem(me - 2 * step + count, count)
            block = whole.at[owner]
            copy_to(block, block, sems, (2 * step,), {"tp": mate}).wait_recv()
            sent.append(copy_to(block, block, sems, (2 * step - 1,), {"tp": mate}))
            sent[-1].start()
        return sent

    def collect(whole, sems):
        for step in range(chips):
            owner = lax.rem(mate - 2 * step + count, count)
            block = whole.at[owner]
            slot = 0 if step == 0 else 2 * step - 1
            copy_to(block, block, sems, (slot,), {"tp": mate}).wait_recv()

    if carried_by_hand:
        for kind in range(4):
            if kind == 3:
                send_across(3, 0)
            for way in (1, -1):
                send_along(kind, 0, col, True, way)
            if kind < 3:
                send_across(kind, 0)
            own(kind).start()
    else:
        for ref, whole, at in ((gate_ref, gate_w, 0), (up_ref, up_w, 1)):
            pltpu.make_async_copy(ref, whole, local_sems.at[at]).start()
        pltpu.make_async_copy(down_ref, down_w.at[0], local_sems.at[2]).start()
    own_weight = pltpu.make_async_copy(projection_ref, weight.at[me], local_sems.at[4])
    own_weight.start()
    sent = spread(projection_ref, weight, proj_sems)

    memory[...] = jnp.zeros_like(memory)
    aux[...] = jnp.zeros_like(aux)
    aux[heads : 2 * heads, :] = jnp.full((heads, DQK), LOWEST_LOG, jnp.float32)
    for step in range(ranks - 1, 0, -1):

        @pl.when(sp >= step)
        def _():
            for copy in state_copies(step):
                copy.wait_recv()
            late = aux_slots[step - 1]
            for head in range(heads):
                rows = pl.ds(head * DV, DV)
                early_max = aux[heads + head : heads + head + 1, :]
                late_max = late[heads + head : heads + head + 1, :]
                late_decay = late[2 * heads + head : 2 * heads + head + 1, :]
                joined = jnp.maximum(late_decay + early_max, late_max)
                before = jnp.exp(late_decay + early_max - joined)
                after = jnp.exp(late_max - joined)
                memory[rows, :] = before * memory[rows, :] + after * slots[
                    step - 1, rows, :
                ].astype(jnp.float32)
                aux[head : head + 1, :] = (
                    before * aux[head : head + 1, :] + after * late[head : head + 1, :]
                )
                aux[heads + head : heads + head + 1, :] = joined
                aux[2 * heads + head : 2 * heads + head + 1, :] = (
                    aux[2 * heads + head : 2 * heads + head + 1, :] + late_decay
                )

    if carried_by_hand:
        crossed(3, 0).wait_recv()
        for way in (1, -1):
            send_along(3, 0, other, False, way)
        stage(1, (0,))

    tile = rows_all // 3
    for head in range(heads):
        prior_max = aux[heads + head : heads + head + 1, :]
        start_max = jnp.maximum(aux[2 * heads + head : 2 * heads + head + 1, :], prior_max)
        lift = jnp.exp(prior_max - start_max) * DQK ** (-0.5)
        memory[head * DV : (head + 1) * DV, :] = memory[head * DV : (head + 1) * DV, :] * lift
        aux[head : head + 1, :] = aux[head : head + 1, :] * lift
        aux[2 * heads + head : 2 * heads + head + 1, :] = start_max

    def read(at, unused):
        start = pl.multiple_of(at * tile, tile)
        rows = pl.ds(start, tile)
        causal = start + lax.broadcasted_iota(
            jnp.int32, (tile, rows_all), 0
        ) >= lax.broadcasted_iota(jnp.int32, (tile, rows_all), 1)
        for head in range(heads):
            keys = slice(head * DQK, (head + 1) * DQK)
            values = slice(head * DV, (head + 1) * DV)
            query = query_ref[rows, keys]
            total = cum_col[rows, head : head + 1]
            spread_log = total - cum_row[head : head + 1, :] + in_row[head : head + 1, :]
            spread_log = jnp.where(causal, spread_log, -jnp.inf)
            carried = total + aux[2 * heads + head : 2 * heads + head + 1, :1]
            running = jnp.maximum(carried, jnp.max(spread_log, axis=-1, keepdims=True))
            scores = lax.dot_general(
                query, key_ref[:, keys], (((1,), (1,)), ((), ())),
                preferred_element_type=jnp.float32,
            ) * DQK ** (-0.5)
            weights = jnp.exp(spread_log - running) * scores
            scaled = jnp.exp(carried - running)
            wide = query.astype(jnp.float32)
            numerator = jnp.dot(
                weights.astype(jnp.bfloat16), value_ref[:, values],
                preferred_element_type=jnp.float32,
            ) + scaled * lax.dot_general(
                wide, memory[values, :], (((1,), (1,)), ((), ())), precision=HIGHEST,
                preferred_element_type=jnp.float32,
            )
            denominator = jnp.sum(weights, axis=-1, keepdims=True) + scaled * jnp.sum(
                wide * aux[head : head + 1, :], axis=-1, keepdims=True
            )
            cell = numerator / jnp.maximum(jnp.abs(denominator), jnp.exp(-running))
            centered = cell - jnp.mean(cell, axis=-1, keepdims=True)
            cell = centered * lax.rsqrt(
                jnp.mean(centered * centered, axis=-1, keepdims=True) + EPSILON
            )
            cell = cell * head_gain[:, values]
            gate = ogate_ref[rows, values].astype(jnp.float32)
            gated[rows, values] = (cell * jax.nn.sigmoid(gate)).astype(jnp.bfloat16)
        return unused

    lax.fori_loop(0, 3, read, 0)
    sent += spread(gated, blocks, gated_sems)
    blocks[me] = gated[...]
    if carried_by_hand:
        stage(1, (1, 2, 3))
    sent += relay(weight, proj_sems)
    if carried_by_hand:
        stage(2, (0, 1))
    sent += relay(blocks, gated_sems)
    collect(weight, proj_sems)
    own_weight.wait()
    collect(blocks, gated_sems)

    def turn(at, unused):
        rows = pl.ds(pl.multiple_of(at * tile, tile), tile)
        mixed = jnp.zeros((tile, width), jnp.float32)
        for block in range(count):
            mixed = mixed + jnp.dot(
                blocks[block, rows, :], weight[block], preferred_element_type=jnp.float32
            )
        scale = lax.rsqrt(jnp.mean(mixed * mixed, axis=-1, keepdims=True) + EPSILON)
        total = residual_ref[rows, :].astype(jnp.float32) + mixed * scale * out_gain[...]
        total = total.astype(jnp.bfloat16)
        first[rows, :] = total
        wide = total.astype(jnp.float32)
        scale = lax.rsqrt(jnp.mean(wide * wide, axis=-1, keepdims=True) + EPSILON)
        normed[rows, :] = (wide * scale * in_gain[...]).astype(jnp.bfloat16)
        return unused

    lax.fori_loop(0, 3, turn, 0)

    if carried_by_hand:
        stage(2, (2, 3))
        stage(3, (0, 1, 2))
        finish((0, 1))
        own(0).wait()
        own(1).wait()
    else:
        for ref, whole, at in ((gate_ref, gate_w, 0), (up_ref, up_w, 1)):
            pltpu.make_async_copy(ref, whole, local_sems.at[at]).wait()

    def mix(at, unused):
        rows = pl.ds(pl.multiple_of(at * tile, tile), tile)
        left = normed[rows, :]
        gate = jnp.dot(left, gate_w[...], preferred_element_type=jnp.float32)
        up = jnp.dot(left, up_w[...], preferred_element_type=jnp.float32)
        active[rows, :] = (gate / (1.0 + jnp.exp(-gate)) * up).astype(jnp.bfloat16)
        return unused

    lax.fori_loop(0, 3, mix, 0)
    if carried_by_hand:
        stage(3, (3,))
        finish((2, 3))
        own(2).wait()
        own(3).wait()
    else:
        pltpu.make_async_copy(down_ref, down_w.at[0], local_sems.at[2]).wait()

    def term(target):
        if carried_by_hand:
            each = cols // down_w.shape[2]
            return jnp.concatenate(
                [
                    jnp.dot(active[...], down_w[target * each + at],
                            preferred_element_type=jnp.float32)
                    for at in range(each)
                ],
                axis=1,
            )
        start = pl.multiple_of(target * cols, cols)
        return jnp.dot(
            active[...], down_w[0, :, pl.ds(start, cols)], preferred_element_type=jnp.float32
        )

    def send(source, target, kind, at, peer):
        return copy_to(source.at[at], target.at[at], sum_sems.at[kind], (at,), {"tp": peer})

    copies = []
    for step in range(1, chips):
        away = lax.rem(me + 2 * step, count)
        to_core[step] = term(away + 1 - 2 * core).astype(jnp.bfloat16)
        hop = send(to_core, from_core, 0, step, mate)
        hop.start()
        mine = term(away)
        hop.wait_recv()
        to_chip[step] = (mine + from_core[step].astype(jnp.float32)).astype(jnp.bfloat16)
        far = send(to_chip, from_chip, 1, step, away)
        far.start()
        copies += [hop, far]
    to_core[0] = term(mate).astype(jnp.bfloat16)
    hop = send(to_core, from_core, 0, 0, mate)
    hop.start()
    result = term(me)
    hop.wait_recv()
    result = result + from_core[0].astype(jnp.float32)
    for far in copies[1::2]:
        far.wait_recv()
    for step in range(1, chips):
        result = result + from_chip[step].astype(jnp.float32)
    own_first = first[:, pl.ds(pl.multiple_of(me * cols, cols), cols)]
    out_ref[...] = (own_first.astype(jnp.float32) + 0.5 * result).astype(jnp.bfloat16)
    for copy in copies + [hop] + sent:
        copy.wait_send()
    for condition, copy in pending:
        when(condition, copy.wait_send)
    for step in range(1, ranks):

        @pl.when(sp + step < ranks)
        def _():
            for copy in state_copies(step):
                copy.wait_send()


def layer(states, logs, cell_inputs, residual, gains, weights):
    decay, memory, normalizer, maximum = states
    running_log_total, in_logs = logs
    ranks, count = lax.axis_size("sp"), lax.axis_size("tp")
    heads = decay.shape[0]
    rows, width = residual.shape
    projection, gate_weight, up_weight, down_weight = weights
    hidden = gate_weight.shape[1]
    inner = projection.shape[0]
    carried_by_hand = ranks == 8
    if carried_by_hand:
        down_shape = (ranks, hidden, down_weight.shape[1])
    else:
        gate_weight = lax.all_gather(gate_weight, "sp", axis=0, tiled=True)
        up_weight = lax.all_gather(up_weight, "sp", axis=0, tiled=True)
        down_weight = lax.all_gather(down_weight, "sp", axis=1, tiled=True)
        down_shape = (1, hidden, width)
    fill = lambda row: jnp.broadcast_to(row[:, None], (heads, DQK))
    aux = jnp.concatenate([normalizer, fill(maximum), fill(decay)])
    height = -(-3 * heads // 8) * 8
    aux = jnp.pad(aux, ((0, height - 3 * heads), (0, 0)))
    low = memory.reshape(heads * DV, DQK).astype(jnp.bfloat16)
    chips, cols, depth = count // 2, width // count, ranks // 2
    buffer = pltpu.VMEM((chips, rows, cols), jnp.bfloat16)
    dma = pltpu.SemaphoreType.DMA
    return pl.pallas_call(
        functools.partial(layer_kernel, ranks, count, heads, carried_by_hand),
        out_shape=jax.ShapeDtypeStruct((rows, cols), jnp.bfloat16),
        in_specs=[VMEM] * 13 + [ANY] * 4,
        out_specs=VMEM,
        scratch_shapes=[
            pltpu.VMEM((ranks - 1, heads * DV, DQK), jnp.bfloat16),
            pltpu.VMEM((ranks - 1, height, DQK), jnp.float32),
            pltpu.VMEM((heads * DV, DQK), jnp.float32),
            pltpu.VMEM((height, DQK), jnp.float32),
            pltpu.VMEM((width, hidden), jnp.bfloat16),
            pltpu.VMEM((width, hidden), jnp.bfloat16),
            pltpu.VMEM(down_shape, jnp.bfloat16),
            pltpu.VMEM((count, inner, width), jnp.bfloat16),
            pltpu.VMEM((rows, inner), jnp.bfloat16),
            pltpu.VMEM((count, rows, inner), jnp.bfloat16),
            pltpu.VMEM((rows, width), jnp.bfloat16),
            pltpu.VMEM((rows, width), jnp.bfloat16),
            pltpu.VMEM((rows, hidden), jnp.bfloat16),
            buffer, buffer, buffer, buffer,
            dma((2, ranks - 1)),
            dma((2, ranks - 1)),
            dma((2, 4, 2, depth, 2)),
            dma((2, 4, 2 * depth - 1)),
            dma((5,)),
            dma((2, count)),
            dma((2, count)),
            dma((2, 2, chips)),
        ],
        compiler_params=pltpu.CompilerParams(
            collective_id=0, has_side_effects=True, vmem_limit_bytes=VMEM_BYTES
        ),
        name="layer",
    )(
        low, aux, running_log_total, in_logs, running_log_total.T, *cell_inputs, residual,
        *gains, projection, gate_weight, up_weight, down_weight,
    )


def body(
    residual,
    query_matrix,
    key_matrix,
    value_matrix,
    output_gate_logit,
    input_gate_log,
    forget_gate_logit,
    extra_head_decay,
    head_norm_gain,
    projection,
    cell_output_gain,
    mixer_input_gain,
    mixer_gate_weight,
    mixer_up_weight,
    mixer_down_weight,
):
    heads_here = input_gate_log.shape[1]
    key_low = heads_first(key_matrix, heads_here, DQK)
    value_low = heads_first(value_matrix, heads_here, DV)
    keyed = key_low.astype(jnp.float32)
    valued = value_low.astype(jnp.float32)
    in_logs = input_gate_log.T
    running_log_total = jnp.cumsum(
        (jax.nn.log_sigmoid(forget_gate_logit) + extra_head_decay).T, axis=-1
    )
    zero_memory = jnp.zeros((heads_here, DV, DQK), jnp.float32)
    zero_normalizer = jnp.zeros((heads_here, DQK), jnp.float32)
    lowest = jnp.full((heads_here,), LOWEST_LOG, jnp.float32)
    local_memory, local_normalizer, local_max = fold_state(
        keyed, valued, in_logs, running_log_total, zero_memory, zero_normalizer, lowest
    )
    return layer(
        (running_log_total[:, -1], local_memory, local_normalizer, local_max),
        (running_log_total, in_logs),
        (query_matrix, key_matrix, value_matrix, output_gate_logit, head_norm_gain[None]),
        residual,
        (cell_output_gain[None], mixer_input_gain[None]),
        (projection, mixer_gate_weight, mixer_up_weight, mixer_down_weight),
    )


def solution(mesh):
    return jax.shard_map(
        body,
        mesh=mesh,
        in_specs=(
            P("sp", None),
            P("sp", "tp"),
            P("sp", "tp"),
            P("sp", "tp"),
            P("sp", "tp"),
            P("sp", "tp"),
            P("sp", "tp"),
            P("sp", "tp"),
            P("tp"),
            P("tp", None),
            P(),
            P(),
            P("sp", "tp"),
            P("sp", "tp"),
            P("tp", "sp"),
        ),
        out_specs=P("sp", "tp"),
        check_vma=False,
    )
```
